32 devices in a mesh: sp: 8 (over z, x), tp: 4 (over y, core).
Axes of the slice: x: 2, y: 2, z: 4, core: 2. Of those that a mesh axis runs over, the one named last changes fastest.
Arguments:
- resid: bfloat16 [6144, 3072], P('sp', 'tp'), may hold values from -12 to 12
- query: bfloat16 [6144, 1536], P('sp', 'tp'), may hold values from -6 to 6
- keys: bfloat16 [6144, 1536], P('sp', 'tp'), may hold values from -6 to 6
- values: bfloat16 [6144, 1536], P('sp', 'tp'), may hold values from -6 to 6
- out_gate: bfloat16 [6144, 1536], P('sp', 'tp'), may hold values from -6 to 6
- in_gate: float32 [16, 6144], P('tp', 'sp'), may hold values from -6 to 110
- forget: float32 [16, 6144], P('tp', 'sp'), may hold values from -1 to 16
- doc_ids: int32 [6144], P('sp'), may hold values from 0 to 3, never falling along the last dimension, each value on 1 to 3072 neighbouring positions
- head_gain: float32 [1536], P('tp'), may hold values from 0.1 to 1.9
- w_out: bfloat16 [1536, 3072], P('tp'), may hold values from -0.15625 to 0.15625
- ffn_gain: float32 [3072], replicated, may hold values from 0.1 to 1.9
- w_gate: bfloat16 [3072, 8448], P('sp', 'tp'), may hold values from -0.109375 to 0.109375
- w_value: bfloat16 [3072, 8448], P('sp', 'tp'), may hold values from -0.109375 to 0.109375
- conv_taps: float32 [3, 8448], P(None, 'tp'), may hold values from -3.5 to 3.5
- w_down: bfloat16 [8448, 3072], P('tp', 'sp'), may hold values from -0.0625 to 0.0625
Outputs:
- layer_out: bfloat16 [6144, 3072], P('sp', 'tp')
The draws below stay inside these ranges and needn't reach their ends.
Inputs may be any that keep to these rules, and one draw needn't show every extreme that they name: `doc_ids`: document numbers never fall along the positions; each document is 1 to 3072 positions long.
All inputs are finite; a program needn't handle non-finite values.
Results may differ from the reference program's by a relative error of at most 0.02.
Values may be sent and summed in bfloat16 or wider, within the bound.
A program may use at most 128 MiB of HBM per device.

```python
import math
import jax
import jax.numpy as jnp
import numpy as np
from jax import lax

D = 3072
H = 16
DH = 96
FF = 8448
BLOCK = 64
TAPS = 3
TOK_DEV = 768
TOKENS = 6144
DOCS = 4
N_TP = 4


def draw_resid(key, part):
    base = jnp.clip(jax.random.normal(key, (TOKENS, D), jnp.float32), -6.0, 6.0)
    phase = jax.random.uniform(jax.random.fold_in(key, 1), (), jnp.float32, 0.0, 6.2832)
    columns = jnp.arange(D, dtype=jnp.float32)
    scale = 0.35 * jnp.exp(0.6 * jnp.sin(6.2832 * columns / D + phase))
    return (base * scale).astype(jnp.bfloat16)


def draw_in_gate(key, part):
    base = jnp.clip(jax.random.normal(key, (H, TOKENS), jnp.float32), -6.0, 6.0)
    return base


def draw_forget(key, part):
    limit = 4
    quick = jax.random.randint(jax.random.fold_in(key, 1), (H, 1), 0, 8) < limit
    rate = jnp.where(quick, 1.0 / 40.0, 1.0 / (4.0 * TOK_DEV))
    factor = jnp.exp(jax.random.uniform(jax.random.fold_in(key, 2), (H, TOKENS // 128), jnp.float32, -1.05, 1.05))
    factor = jnp.repeat(factor, 128, axis=1)
    noise = 0.5 * jnp.clip(jax.random.normal(jax.random.fold_in(key, 3), (H, TOKENS), jnp.float32), -6.0, 6.0)
    return -jnp.log(rate * factor) + noise


def steps_of(stream_key, extent, cuts, least, top_value):
    def one(position, blocks):
        draws = jax.random.uniform(jax.random.fold_in(jax.random.fold_in(stream_key, 6), position), (blocks,), jnp.float32, least / len(cuts), top_value / len(cuts))
        return jnp.repeat(jnp.exp(draws), extent[position] // blocks).reshape((-1,) + (1,) * (len(extent) - position - 1))

    gain = one(*cuts[0])
    for cut in cuts[1:]:
        gain = gain * one(*cut)
    return gain


def length_profile(count, total, most, skew):
    loads = [(1 << 20) // math.isqrt(rank ** skew) + 1 for rank in range(2, count + 1)]
    spare, counts = total - most - (count - 1), [1] * (count - 1)
    while spare > 0:
        free = [i for i in range(count - 1) if counts[i] < most]
        mass, remaining = sum([loads[i] for i in free]), spare
        for i in free:
            addition = min(most - counts[i], max(1, remaining * loads[i] // mass), spare)
            counts[i] = counts[i] + addition
            spare = spare - addition
    return np.array([most] + counts)


def uneven(stream_key, amount, total, reach, skew):
    if amount == 2:
        one = jax.random.randint(stream_key, (), max(1, total - reach), min(reach, total - 1) + 1)
        return jnp.stack([one, total - one])
    sizes = jnp.asarray(length_profile(amount, total, reach, skew), jnp.int32)
    pairs = (amount - 1) // 2
    giver, taker = sizes[1:1 + 2 * pairs:2], sizes[2:2 + 2 * pairs:2]
    margin = jnp.minimum(giver - 1, reach - taker)
    moved = jax.random.randint(jax.random.fold_in(stream_key, 1), (pairs,), 0, 1 << 20) % (margin + 1)
    sizes = sizes.at[1:1 + 2 * pairs:2].set(giver - moved).at[2:2 + 2 * pairs:2].set(taker + moved)
    return sizes[jax.random.permutation(jax.random.fold_in(stream_key, 2), amount)]


def centred(rng, dims, scale, most, shards=(), held_as=jnp.bfloat16):
    gain = steps_of(rng, dims, shards, -0.22, 0.18) if shards else 1.0
    entries = jax.random.normal(rng, dims, jnp.float32) * scale * gain
    return jnp.minimum(jnp.maximum(entries, -most), most).astype(held_as)


def setup_inputs(seed: int = 0) -> dict:
    splits = jax.random.split(jax.random.key(seed), 16)
    return {
        "resid": draw_resid(jax.random.fold_in(splits[15], 71), 0),
        "query": centred(splits[1], (TOKENS, H * DH), 1.0, 6.0, ((0, 8), (1, 4))),
        "keys": centred(splits[2], (TOKENS, H * DH), 1.0, 6.0, ((0, 8), (1, 4))),
        "values": centred(splits[3], (TOKENS, H * DH), 1.0, 6.0, ((0, 8), (1, 4))),
        "out_gate": centred(splits[4], (TOKENS, H * DH), 1.0, 6.0, ((0, 8), (1, 4))),
        "in_gate": draw_in_gate(jax.random.fold_in(splits[15], 71), 0),
        "forget": draw_forget(jax.random.fold_in(splits[15], 71), 0),
        "doc_ids": jnp.searchsorted(jnp.cumsum(uneven(splits[7], DOCS, TOKENS, 4 * TOK_DEV, 0)), jnp.arange(TOKENS), side="right").astype(jnp.int32),
        "head_gain": jnp.clip(1.0 + 0.18 * jax.random.normal(splits[8], (H * DH,), jnp.float32), 0.1, 1.9),
        "w_out": centred(splits[9], (H * DH, D), (H * DH) ** -0.5, 0.15625, ((0, 4),)),
        "ffn_gain": jnp.clip(1.0 + 0.18 * jax.random.normal(splits[10], (D,), jnp.float32), 0.1, 1.9),
        "w_gate": centred(splits[11], (D, FF), D ** -0.5, 0.109375, ((0, 8), (1, 4))),
        "w_value": centred(splits[12], (D, FF), D ** -0.5, 0.109375, ((0, 8), (1, 4))),
        "conv_taps": centred(splits[13], (TAPS, FF), TAPS ** -0.5, 3.5, ((1, 4),), jnp.float32),
        "w_down": centred(splits[14], (FF, D), FF ** -0.5, 0.0625, ((0, 4), (1, 8))),
    }


ABSENT = -1e+30
epsilon = 1e-06
head_floor = 1.0
HIGHEST = lax.Precision.HIGHEST

def combine(early, late):
    state_early, peak_early, decay_early, first_early, last_early, second_early = early
    state_late, peak_late, decay_late, first_late, last_late, second_late = late
    early_empty = last_early < 0.0
    late_empty = first_late < 0.0
    cut = (first_late != last_early) & jnp.logical_not(early_empty) & jnp.logical_not(late_empty)
    passed = jnp.where(cut, ABSENT, decay_late)
    peak = jnp.maximum(passed + peak_early, peak_late)
    keep = jnp.exp(passed + peak_early - peak)
    fresh = jnp.exp(peak_late - peak)
    state = keep[..., None, None] * state_early + fresh[..., None, None] * state_late
    return (state, peak, decay_early + passed, jnp.where(early_empty, first_late, first_early), jnp.where(late_empty, last_early, last_late), jnp.where(late_empty, second_early, second_late))

def empty_state(heads, width):
    return (jnp.zeros((heads, width, width), jnp.float32), jnp.full((heads,), ABSENT, jnp.float32), jnp.zeros((heads,), jnp.float32), jnp.full((1,), -1.0, jnp.float32), jnp.full((1,), -1.0, jnp.float32), jnp.full((1,), -1.0, jnp.float32))

def advance(carry, item):
    return (combine(carry, item), carry)

def block_parts(query, keys, values, in_gate, forget, seg):
    length, heads, width = query.shape
    count = length // BLOCK
    query_blocks = query.reshape(count, BLOCK, heads, width)
    key_blocks = (keys * width ** (-0.5)).reshape(count, BLOCK, heads, width)
    value_blocks = values.reshape(count, BLOCK, heads, width)
    gate_in = in_gate.T.reshape(count, BLOCK, heads)
    cumul = jnp.cumsum(jax.nn.log_sigmoid(forget.T).reshape(count, BLOCK, heads), axis=1)
    seg_blocks = seg.reshape(count, BLOCK)
    total = cumul[:, -1]
    in_last = (seg_blocks == seg_blocks[:, -1:])[:, :, None]
    weight_log = jnp.where(in_last, total[:, None] - cumul + gate_in, ABSENT)
    local_peak = lax.optimization_barrier(jnp.max(weight_log, axis=1))
    weights = jnp.exp(weight_log - local_peak[:, None])
    update = jnp.einsum('nchk,nchv->nhkv', weights[..., None] * key_blocks, value_blocks, precision=HIGHEST)
    whole = jnp.all(seg_blocks == seg_blocks[:, :1], axis=1)[:, None]
    decay = jnp.where(whole, total, ABSENT)
    elements = (update, local_peak, decay, seg_blocks[:, :1], seg_blocks[:, -1:], seg_blocks[:, -2:-1])
    return (elements, (query_blocks, key_blocks, value_blocks, gate_in, cumul, seg_blocks))

def block_outputs(before, parts):
    state, peak_prev, _, _, last_prev, _ = before
    query_blocks, key_blocks, value_blocks, gate_in, cumul, seg_blocks = parts
    count, span, heads, width = query_blocks.shape
    carried = (seg_blocks == last_prev)[:, :, None]
    inter = jnp.where(carried, cumul + peak_prev[:, None], ABSENT)
    places = jnp.arange(span)
    causal = (places[:, None] >= places[None, :])[None, :, :, None]
    same = (seg_blocks[:, :, None] == seg_blocks[:, None, :])[..., None]
    diff_log = jnp.where(causal & same, cumul[:, :, None] - cumul[:, None] + gate_in[:, None], ABSENT)
    top = jnp.maximum(inter, lax.optimization_barrier(jnp.max(diff_log, axis=2)))
    scores = jnp.einsum('nthd,nshd->ntsh', query_blocks, key_blocks, precision=HIGHEST) * jnp.exp(diff_log - top[:, :, None])
    result = jnp.einsum('ntsh,nshd->nthd', scores, value_blocks, precision=HIGHEST)
    result = result + jnp.exp(inter - top)[..., None] * jnp.einsum('nthk,nhkv->nthv', query_blocks, state, precision=HIGHEST)
    return result.reshape(count * span, heads, width)

def reference(resid, query, keys, values, out_gate, in_gate, forget, doc_ids, head_gain, w_out, ffn_gain, w_gate, w_value, conv_taps, w_down):
    length = query.shape[0]
    seg = doc_ids.astype(jnp.float32)
    query_f = query.astype(jnp.float32).reshape(length, H, DH)
    keys_f = keys.astype(jnp.float32).reshape(length, H, DH)
    values_f = values.astype(jnp.float32).reshape(length, H, DH)
    elements, parts = block_parts(query_f, keys_f, values_f, in_gate, forget, seg)
    _, before = lax.scan(advance, empty_state(H, DH), elements)
    memory_out = block_outputs(before, parts)
    normed = memory_out * lax.rsqrt(lax.optimization_barrier(jnp.mean(memory_out * memory_out, axis=-1, keepdims=True)) + head_floor)
    normed = normed.reshape(length, H * DH) * head_gain * jax.nn.sigmoid(out_gate.astype(jnp.float32))
    mix = normed.astype(jnp.bfloat16)
    width_group = H // N_TP * DH
    attended = jnp.zeros((length, D), jnp.float32)
    for index in range(N_TP):
        share = jnp.dot(mix[:, index * width_group:(index + 1) * width_group], w_out[index * width_group:(index + 1) * width_group], preferred_element_type=jnp.float32).astype(jnp.bfloat16)
        attended = attended + lax.optimization_barrier(share).astype(jnp.float32)
    residual_one = resid.astype(jnp.float32) + attended
    scale = lax.rsqrt(lax.optimization_barrier(jnp.mean(residual_one * residual_one, axis=1, keepdims=True)) + epsilon)
    normed_rows = (residual_one * scale * ffn_gain).astype(jnp.bfloat16)
    gate = jnp.dot(normed_rows, w_gate, preferred_element_type=jnp.float32).astype(jnp.bfloat16)
    value = jnp.dot(normed_rows, w_value, preferred_element_type=jnp.float32).astype(jnp.bfloat16)
    extended = jnp.concatenate([jnp.zeros((2, FF), jnp.bfloat16), gate], axis=0).astype(jnp.float32)
    ids = jnp.concatenate([jnp.full((2,), -1.0, jnp.float32), seg])
    near = (ids[1:-1] == seg)[:, None]
    far = (ids[:-2] == seg)[:, None]
    conv = conv_taps[2] * extended[2:] + conv_taps[1] * jnp.where(near, extended[1:-1], 0.0) + conv_taps[0] * jnp.where(far, extended[:-2], 0.0)
    hidden = (jax.nn.silu(conv) * value.astype(jnp.float32)).astype(jnp.bfloat16)
    group = FF // N_TP
    down = jnp.zeros((length, D), jnp.float32)
    for index in range(N_TP):
        partial_rows = jnp.dot(hidden[:, index * group:(index + 1) * group], w_down[index * group:(index + 1) * group], preferred_element_type=jnp.float32).astype(jnp.bfloat16)
        down = down + lax.optimization_barrier(partial_rows).astype(jnp.float32)
    return (residual_one + down).astype(jnp.bfloat16)
```

```python
import jax
import jax.numpy as jnp
from jax import lax
from jax.sharding import PartitionSpec as P

DH = 96
ABSENT = -1e30
epsilon = 1e-06
head_floor = 1.0


def memory_local(query, keys, values, in_gate, cumul, seg):
    tokens = query.shape[0]
    heads = in_gate.shape[0]
    place = jnp.arange(tokens)
    allowed = (place[:, None] >= place[None, :]) & (seg[:, None] == seg[None, :])
    log = jnp.where(
        allowed[None], cumul[:, :, None] - cumul[:, None, :] + in_gate[:, None, :], ABSENT
    )
    top = jnp.max(log, axis=2)
    results = []
    for h in range(heads):
        part = slice(h * DH, (h + 1) * DH)
        scores = lax.dot_general(
            query[:, part], keys[:, part], (((1,), (1,)), ((), ())),
            preferred_element_type=jnp.float32,
        )
        scores = scores * jnp.exp(log[h] - top[h][:, None]) * DH ** (-0.5)
        results.append(
            jnp.dot(
                scores.astype(jnp.bfloat16), values[:, part], preferred_element_type=jnp.float32
            )
        )
    return results, top


def memory_state(keys, values, in_gate, cumul, seg):
    heads = in_gate.shape[0]
    log = jnp.where(seg[None] == seg[-1], cumul[:, -1:] - cumul + in_gate, ABSENT)
    peak = jnp.max(log, axis=1)
    weight = jnp.exp(log - peak[:, None])
    states = []
    for h in range(heads):
        part = slice(h * DH, (h + 1) * DH)
        weighted = (keys[:, part].astype(jnp.float32) * weight[h][:, None]).astype(jnp.bfloat16)
        states.append(
            lax.dot_general(
                weighted, values[:, part], (((0,), (0,)), ((), ())),
                preferred_element_type=jnp.float32,
            )
        )
    return jnp.stack(states) * DH ** (-0.5), peak


def body(
    resid,
    query,
    keys,
    values,
    out_gate,
    in_gate,
    forget,
    doc_ids,
    head_gain,
    w_out,
    ffn_gain,
    w_gate,
    w_value,
    conv_taps,
    w_down,
):
    tokens = query.shape[0]
    heads = query.shape[1] // DH
    count = lax.axis_size("sp")
    me = lax.axis_index("sp")
    across = count // 4
    side = (me // across) % 2
    first = side == 0
    column = me % across
    hidden_units = w_gate.shape[1]
    half = hidden_units // 2
    width = w_gate.shape[0] * count

    def flip(value, bit):
        return lax.ppermute(value, "sp", [(s, s ^ bit) for s in range(count)])

    def shift(value, by):
        return lax.ppermute(
            value,
            "sp",
            [(s, s - s % across + (s % across + by) % across) for s in range(count)],
        )

    def halves(w, axis):
        low = lax.slice_in_dim(w, 0, half, axis=axis)
        high = lax.slice_in_dim(w, half, hidden_units, axis=axis)
        return jnp.where(first, low, high), jnp.where(first, high, low)

    def collect(own, other):
        near = flip(other, across)
        far = flip(own, 2 * across)
        far_near = flip(near, 2 * across)
        blocks = []
        for block, bits in (
            (own, 0),
            (near, across),
            (far, 2 * across),
            (far_near, 3 * across),
        ):
            blocks.append((block, me ^ bits))
            for by in range(1, across):
                source = me - column + (column - by + across) % across
                blocks.append((shift(block, by), source ^ bits))
        return blocks

    gate_own, gate_other = halves(w_gate, 1)
    value_own, value_other = halves(w_value, 1)
    down_own, down_other = halves(w_down, 0)
    up_blocks = collect(
        jnp.concatenate([gate_own, value_own], axis=1),
        jnp.concatenate([gate_other, value_other], axis=1),
    )
    down_blocks = collect(down_own, down_other)

    seg = doc_ids.astype(jnp.float32)
    cumul = jnp.cumsum(jax.nn.log_sigmoid(forget), axis=1)
    state, peak = memory_state(keys, values, in_gate, cumul, seg)

    def row(x):
        return jnp.broadcast_to(x[:, None, None], (heads, 1, DH))

    def same(x):
        return jnp.broadcast_to(x, (heads, 1, DH))

    packed = jnp.concatenate(
        [
            state,
            row(peak),
            row(cumul[:, -1]),
            same(seg[-1]),
            same(seg[-2]),
            jnp.zeros((heads, 4, DH), jnp.float32),
        ],
        axis=1,
    )
    everything = lax.all_gather(packed, "sp")
    local, top = memory_local(query, keys, values, in_gate, cumul, seg)
    peaks = everything[:, :, DH, 0]
    totals = everything[:, :, DH + 1, 0]
    lasts = everything[:, 0, DH + 2, 0]
    seconds = everything[:, 0, DH + 3, 0]
    place = jnp.arange(count)
    before = place == me - 1
    last_prev = jnp.sum(jnp.where(before, lasts + 1.0, 0.0)) - 1.0
    second_prev = jnp.sum(jnp.where(before, seconds + 1.0, 0.0)) - 1.0
    within = (place[:, None] < place[None, :]) & (place[None, :] < me)
    passed = jnp.sum(jnp.where(within[:, :, None], totals[None], 0.0), axis=1)
    use = ((place < me) & (lasts == last_prev))[:, None]
    logs = jnp.where(use, peaks + passed, ABSENT)
    peak_in = jnp.max(logs, axis=0)
    coef = jnp.where(use, jnp.exp(logs - peak_in[None]), 0.0)
    state_in = jnp.sum(coef[:, :, None, None] * everything[:, :, :DH], axis=0)
    inter = jnp.where((seg == last_prev)[None], cumul + peak_in[:, None], ABSENT)
    peak_all = jnp.maximum(inter, top)
    keep_local = jnp.exp(top - peak_all)
    keep_inter = jnp.exp(inter - peak_all)
    normed = []
    for h in range(heads):
        part = slice(h * DH, (h + 1) * DH)
        out = keep_local[h][:, None] * local[h] + keep_inter[h][:, None] * jnp.dot(
            query[:, part],
            state_in[h].astype(jnp.bfloat16),
            preferred_element_type=jnp.float32,
        )
        normed.append(
            out * lax.rsqrt(jnp.mean(out * out, axis=-1, keepdims=True) + head_floor)
        )
    mix = (
        jnp.concatenate(normed, axis=1)
        * head_gain
        * jax.nn.sigmoid(out_gate.astype(jnp.float32))
    ).astype(jnp.bfloat16)

    share = jnp.dot(mix, w_out, preferred_element_type=jnp.float32).astype(jnp.bfloat16)
    local_cols = resid.shape[1]
    attended = lax.psum_scatter(share, "tp", scatter_dimension=1, tiled=True).astype(jnp.float32)
    residual_own = resid.astype(jnp.float32) + attended
    squares = lax.psum(jnp.sum(residual_own * residual_own, axis=1), "tp")
    offset = lax.axis_index("tp") * local_cols
    gains = lax.dynamic_slice_in_dim(ffn_gain, offset, local_cols, 0)
    own_rows = (residual_own * lax.rsqrt(squares[:, None] / width + epsilon) * gains).astype(
        jnp.bfloat16
    )
    rows_mine = lax.all_gather(own_rows, "tp", axis=1, tiled=True)
    rows_theirs = lax.all_gather(flip(own_rows, across), "tp", axis=1, tiled=True)
    ids = jnp.concatenate([second_prev[None], last_prev[None], seg])
    masks = jnp.stack([ids[1:-1] == seg, ids[:-2] == seg]).astype(jnp.float32)
    masks_theirs = flip(masks, across)

    whole_up = jnp.zeros((count,) + up_blocks[0][0].shape, jnp.bfloat16)
    for block, index in up_blocks:
        whole_up = lax.dynamic_update_index_in_dim(whole_up, block, index, 0)
    whole_up = whole_up.reshape(width, 2 * half)
    whole_down = jnp.zeros((count,) + down_blocks[0][0].shape, jnp.bfloat16)
    for block, index in down_blocks:
        whole_down = lax.dynamic_update_index_in_dim(whole_down, block, index, 0)
    whole_down = whole_down.transpose(1, 0, 2).reshape(half, width)

    up_mine = jnp.dot(rows_mine, whole_up, preferred_element_type=jnp.float32).astype(jnp.bfloat16)
    up_theirs = jnp.dot(rows_theirs, whole_up, preferred_element_type=jnp.float32).astype(
        jnp.bfloat16
    )
    edge_mine, edge_theirs = up_mine[-2:, :half], up_theirs[-2:, :half]
    edge_low = jnp.where(first, edge_mine, edge_theirs)
    edge_high = jnp.where(first, edge_theirs, edge_mine)
    got_low = shift(edge_low, 1)
    got_high = lax.ppermute(edge_high, "sp", next_pairs(count, across))
    swap = column == 0
    prev_low = jnp.where(swap, got_high, got_low)
    prev_high = jnp.where(swap, got_low, got_high)
    prev_mine = jnp.where(first, prev_low, prev_high)
    prev_theirs = jnp.where(first, prev_high, prev_low)

    taps_low, taps_high = conv_taps[:, :half], conv_taps[:, half:]
    taps = jnp.where(first, taps_low, taps_high)

    def mixed(up, prev, mask):
        extended = jnp.concatenate([prev, up[:, :half]], axis=0).astype(jnp.float32)
        near = mask[0][:, None] > 0.5
        far = mask[1][:, None] > 0.5
        conv = (
            taps[2] * extended[2:]
            + taps[1] * jnp.where(near, extended[1:-1], 0.0)
            + taps[0] * jnp.where(far, extended[:-2], 0.0)
        )
        return (jax.nn.silu(conv) * up[:, half:].astype(jnp.float32)).astype(jnp.bfloat16)

    def lowered(up, prev, mask):
        hidden = mixed(up, prev, mask)
        terms = jnp.dot(hidden, whole_down, preferred_element_type=jnp.float32)
        return lax.psum_scatter(
            terms.astype(jnp.bfloat16), "tp", scatter_dimension=1, tiled=True
        )

    down_theirs = flip(lowered(up_theirs, prev_theirs, masks_theirs), across)
    down_mine = lowered(up_mine, prev_mine, masks)
    down = down_mine.astype(jnp.float32) + down_theirs.astype(jnp.float32)
    return (residual_own + down).astype(jnp.bfloat16)


def next_pairs(count, across):
    pairs = []
    for s in range(count):
        column, top = s % across, s // (2 * across)
        if column < across - 1:
            pairs.append((s, s + 1))
        elif (top + 1) * 2 * across < count:
            pairs.append((s, s - column + 2 * across))
    return pairs


def solution(mesh):
    placed = (
        P("sp", "tp"),
        P("sp", "tp"),
        P("sp", "tp"),
        P("sp", "tp"),
        P("sp", "tp"),
        P("tp", "sp"),
        P("tp", "sp"),
        P("sp"),
        P("tp"),
        P("tp", None),
        P(),
        P("sp", "tp"),
        P("sp", "tp"),
        P(None, "tp"),
        P("tp", "sp"),
    )
    return jax.shard_map(body, mesh=mesh, in_specs=placed, out_specs=P("sp", "tp"), check_vma=False)
```

```python
import jax
import jax.numpy as jnp
from jax import lax
from jax.experimental import pallas as pl
from jax.experimental.pallas import tpu as pltpu
from jax.sharding import PartitionSpec as P

DH = 96
ABSENT = -1e30
epsilon = 1e-06
head_floor = 1.0


def memory_local(query, keys, values, in_gate, cumul, seg):
    tokens = query.shape[0]
    heads = in_gate.shape[0]
    place = jnp.arange(tokens)
    allowed = (place[:, None] >= place[None, :]) & (seg[:, None] == seg[None, :])
    log = jnp.where(
        allowed[None], cumul[:, :, None] - cumul[:, None, :] + in_gate[:, None, :], ABSENT
    )
    top = jnp.max(log, axis=2)
    results = []
    for h in range(heads):
        part = slice(h * DH, (h + 1) * DH)
        scores = lax.dot_general(
            query[:, part], keys[:, part], (((1,), (1,)), ((), ())),
            preferred_element_type=jnp.float32,
        )
        scores = scores * jnp.exp(log[h] - top[h][:, None]) * DH ** (-0.5)
        results.append(
            jnp.dot(
                scores.astype(jnp.bfloat16),
                values[:, part],
                preferred_element_type=jnp.float32,
            )
        )
    return results, top


def memory_state(keys, values, in_gate, cumul, seg):
    heads = in_gate.shape[0]
    log = jnp.where(seg[None] == seg[-1], cumul[:, -1:] - cumul + in_gate, ABSENT)
    peak = jnp.max(log, axis=1)
    weight = jnp.exp(log - peak[:, None])
    states = []
    for h in range(heads):
        part = slice(h * DH, (h + 1) * DH)
        weighted = (keys[:, part].astype(jnp.float32) * weight[h][:, None]).astype(jnp.bfloat16)
        states.append(
            lax.dot_general(
                weighted, values[:, part], (((0,), (0,)), ((), ())),
                preferred_element_type=jnp.float32,
            )
        )
    return jnp.stack(states) * DH ** (-0.5), peak


def halved(w_gate, w_value, w_down, side):
    units, depth = w_gate.shape
    half = units // 2
    columns = w_down.shape[1]

    def kernel(side_ref, gate, value, down, up_own, up_other, down_own, down_other):
        def give(up_low, up_high, down_low, down_high):
            for k, source in enumerate((gate, value)):
                up_low[k] = source[:half]
                up_high[k] = source[half:]
            down_low[...] = down[:half]
            down_high[...] = down[half:]

        pl.when(side_ref[0] == 0)(lambda: give(up_own, up_other, down_own, down_other))
        pl.when(side_ref[0] != 0)(lambda: give(up_other, up_own, down_other, down_own))

    vmem = pl.BlockSpec(memory_space=pltpu.VMEM)
    up = jax.ShapeDtypeStruct((2, half, depth), jnp.bfloat16)
    down = jax.ShapeDtypeStruct((half, columns), jnp.bfloat16)
    return pl.pallas_call(
        kernel,
        in_specs=[pl.BlockSpec(memory_space=pltpu.SMEM)] + [vmem] * 3,
        out_specs=[vmem] * 4,
        out_shape=[up, up, down, down],
        compiler_params=pltpu.CompilerParams(vmem_limit_bytes=30 << 20),
        name="halved",
    )(side.astype(jnp.int32)[None], w_gate, w_value, w_down)


def raised(rows_mine, rows_theirs, blocks):
    tokens, width = rows_mine.shape
    _, columns, depth = blocks[0][0].shape
    count = len(blocks)
    tile = tokens // 3
    steps = tokens // tile
    index = jnp.stack([place for _, place in blocks]).astype(jnp.int32)

    def kernel(index_ref, mine, theirs, *rest):
        sources = rest[:count]
        gate, value, weights, sems = rest[count:]
        step = pl.program_id(0)

        @pl.when(step == 0)
        def _():
            copies = [
                pltpu.make_async_copy(sources[k], weights.at[index_ref[k]], sems.at[k])
                for k in range(count)
            ]
            for copy in copies:
                copy.start()
            for copy in copies:
                copy.wait()

        def multiply(rows):
            for part, out in enumerate((gate, value)):
                total = None
                for k in range(count):
                    term = lax.dot_general(
                        rows[:, k * depth : (k + 1) * depth],
                        weights[k, part],
                        (((1,), (1,)), ((), ())),
                        preferred_element_type=jnp.float32,
                    )
                    total = term if total is None else total + term
                out[...] = total.astype(jnp.bfloat16)

        pl.when(step < steps)(lambda: multiply(mine))
        pl.when(step >= steps)(lambda: multiply(theirs))

    return pl.pallas_call(
        kernel,
        grid_spec=pltpu.PrefetchScalarGridSpec(
            num_scalar_prefetch=1,
            grid=(2 * steps,),
            in_specs=[
                pl.BlockSpec((tile, width), lambda i, index: (jnp.minimum(i, steps - 1), 0)),
                pl.BlockSpec((tile, width), lambda i, index: (jnp.maximum(i - steps, 0), 0)),
            ]
            + [pl.BlockSpec(memory_space=pl.ANY)] * count,
            out_specs=[pl.BlockSpec((tile, columns), lambda i, index: (i, 0))] * 2,
            scratch_shapes=[
                pltpu.VMEM((count, 2, columns, depth), jnp.bfloat16),
                pltpu.SemaphoreType.DMA((count,)),
            ],
        ),
        out_shape=[jax.ShapeDtypeStruct((2 * tokens, columns), jnp.bfloat16)] * 2,
        compiler_params=pltpu.CompilerParams(vmem_limit_bytes=40 << 20),
        cost_estimate=pl.CostEstimate(
            flops=8 * tokens * width * columns,
            bytes_accessed=2 * (2 * tokens + columns) * width,
            transcendentals=0,
        ),
        name="raised",
    )(index, rows_mine, rows_theirs, *[block for block, _ in blocks])


def down_product(hidden, blocks):
    tokens, depth = hidden.shape
    columns = blocks[0][0].shape[1]
    count = len(blocks)
    tile = tokens // 3
    index = jnp.stack([place for _, place in blocks]).astype(jnp.int32)

    def kernel(index_ref, rows, *rest):
        sources, out, weights, sems = rest[:count], rest[count], rest[count + 1], rest[count + 2]

        @pl.when(pl.program_id(0) == 0)
        def _():
            copies = [
                pltpu.make_async_copy(sources[k], weights.at[index_ref[k]], sems.at[k])
                for k in range(count)
            ]
            for copy in copies:
                copy.start()
            for copy in copies:
                copy.wait()

        for k in range(count):
            out[k] = jnp.dot(
                rows[...], weights[k], preferred_element_type=jnp.float32
            ).astype(jnp.bfloat16)

    return pl.pallas_call(
        kernel,
        grid_spec=pltpu.PrefetchScalarGridSpec(
            num_scalar_prefetch=1,
            grid=(tokens // tile,),
            in_specs=[pl.BlockSpec((tile, depth), lambda i, index: (i, 0))]
            + [pl.BlockSpec(memory_space=pl.ANY)] * count,
            out_specs=pl.BlockSpec((count, tile, columns), lambda i, index: (0, i, 0)),
            scratch_shapes=[
                pltpu.VMEM((count, depth, columns), jnp.bfloat16),
                pltpu.SemaphoreType.DMA((count,)),
            ],
        ),
        out_shape=jax.ShapeDtypeStruct((count, tokens, columns), jnp.bfloat16),
        compiler_params=pltpu.CompilerParams(vmem_limit_bytes=40 << 20),
        cost_estimate=pl.CostEstimate(
            flops=2 * tokens * depth * count * columns,
            bytes_accessed=2 * count * columns * (tokens + depth),
            transcendentals=0,
        ),
        name="lowered",
    )(index, hidden, *[block for block, _ in blocks])


def layer(
    resid,
    query,
    keys,
    values,
    out_gate,
    in_gate,
    forget,
    doc_ids,
    head_gain,
    w_out,
    ffn_gain,
    w_gate,
    w_value,
    conv_taps,
    w_down,
):
    tokens = query.shape[0]
    heads = query.shape[1] // DH
    count = lax.axis_size("sp")
    me = lax.axis_index("sp")
    across = count // 4
    side = (me // across) % 2
    first = side == 0
    column = me % across
    hidden_units = w_gate.shape[1]
    half = hidden_units // 2
    width = w_gate.shape[0] * count

    def flip(value, bit):
        return lax.ppermute(value, "sp", [(s, s ^ bit) for s in range(count)])

    def shift(value, by):
        return lax.ppermute(
            value,
            "sp",
            [(s, s - s % across + (s % across + by) % across) for s in range(count)],
        )

    up_own, up_other, down_own, down_other = halved(w_gate.T, w_value.T, w_down, side)

    def collect(own, other):
        near = flip(other, across)
        far = flip(own, 2 * across)
        far_near = flip(near, 2 * across)
        blocks = []
        for block, bits in (
            (own, 0),
            (near, across),
            (far, 2 * across),
            (far_near, 3 * across),
        ):
            blocks.append((block, me ^ bits))
            for by in range(1, across):
                source = me - column + (column - by + across) % across
                blocks.append((shift(block, by), source ^ bits))
        return blocks

    up_blocks = collect(up_own, up_other)
    down_blocks = collect(down_own, down_other)

    seg = doc_ids.astype(jnp.float32)
    cumul = jnp.cumsum(jax.nn.log_sigmoid(forget), axis=1)
    state, peak = memory_state(keys, values, in_gate, cumul, seg)

    def row(x):
        return jnp.broadcast_to(x[:, None, None], (heads, 1, DH))

    def same(x):
        return jnp.broadcast_to(x, (heads, 1, DH))

    packed = jnp.concatenate(
        [
            state,
            row(peak),
            row(cumul[:, -1]),
            same(seg[-1]),
            same(seg[-2]),
            jnp.zeros((heads, 4, DH), jnp.float32),
        ],
        axis=1,
    )
    everything = lax.all_gather(packed, "sp")
    local, top = memory_local(query, keys, values, in_gate, cumul, seg)
    peaks = everything[:, :, DH, 0]
    totals = everything[:, :, DH + 1, 0]
    lasts = everything[:, 0, DH + 2, 0]
    seconds = everything[:, 0, DH + 3, 0]
    place = jnp.arange(count)
    before = place == me - 1
    last_prev = jnp.sum(jnp.where(before, lasts + 1.0, 0.0)) - 1.0
    second_prev = jnp.sum(jnp.where(before, seconds + 1.0, 0.0)) - 1.0
    within = (place[:, None] < place[None, :]) & (place[None, :] < me)
    passed = jnp.sum(jnp.where(within[:, :, None], totals[None], 0.0), axis=1)
    use = ((place < me) & (lasts == last_prev))[:, None]
    logs = jnp.where(use, peaks + passed, ABSENT)
    peak_in = jnp.max(logs, axis=0)
    coef = jnp.where(use, jnp.exp(logs - peak_in[None]), 0.0)
    state_in = jnp.sum(coef[:, :, None, None] * everything[:, :, :DH], axis=0)
    inter = jnp.where((seg == last_prev)[None], cumul + peak_in[:, None], ABSENT)
    peak_all = jnp.maximum(inter, top)
    keep_local = jnp.exp(top - peak_all)
    keep_inter = jnp.exp(inter - peak_all)
    normed = []
    for h in range(heads):
        part = slice(h * DH, (h + 1) * DH)
        out = keep_local[h][:, None] * local[h] + keep_inter[h][:, None] * jnp.dot(
            query[:, part],
            state_in[h].astype(jnp.bfloat16),
            preferred_element_type=jnp.float32,
        )
        normed.append(
            out * lax.rsqrt(jnp.mean(out * out, axis=-1, keepdims=True) + head_floor)
        )
    mix = (
        jnp.concatenate(normed, axis=1)
        * head_gain
        * jax.nn.sigmoid(out_gate.astype(jnp.float32))
    ).astype(jnp.bfloat16)

    share = jnp.dot(mix, w_out, preferred_element_type=jnp.float32).astype(jnp.bfloat16)
    local_cols = resid.shape[1]
    attended = lax.psum_scatter(share, "tp", scatter_dimension=1, tiled=True).astype(jnp.float32)
    residual_own = resid.astype(jnp.float32) + attended
    squares = lax.psum(jnp.sum(residual_own * residual_own, axis=1), "tp")
    offset = lax.axis_index("tp") * local_cols
    gains = lax.dynamic_slice_in_dim(ffn_gain, offset, local_cols, 0)
    own_rows = (residual_own * lax.rsqrt(squares[:, None] / width + epsilon) * gains).astype(
        jnp.bfloat16
    )
    rows_mine = lax.all_gather(own_rows, "tp", axis=1, tiled=True)
    rows_theirs = lax.all_gather(flip(own_rows, across), "tp", axis=1, tiled=True)
    ids = jnp.concatenate([second_prev[None], last_prev[None], seg])
    masks = jnp.stack([ids[1:-1] == seg, ids[:-2] == seg]).astype(jnp.float32)
    masks_theirs = flip(masks, across)

    gate_both, value_both = raised(rows_mine, rows_theirs, up_blocks)
    gate_mine, gate_theirs = gate_both[:tokens], gate_both[tokens:]
    edge_mine, edge_theirs = gate_mine[-2:], gate_theirs[-2:]
    edge_low = jnp.where(first, edge_mine, edge_theirs)
    edge_high = jnp.where(first, edge_theirs, edge_mine)
    got_low = shift(edge_low, 1)
    got_high = lax.ppermute(edge_high, "sp", next_pairs(count, across))
    swap = column == 0
    prev_low = jnp.where(swap, got_high, got_low)
    prev_high = jnp.where(swap, got_low, got_high)
    prev_mine = jnp.where(first, prev_low, prev_high)
    prev_theirs = jnp.where(first, prev_high, prev_low)

    taps_low, taps_high = conv_taps[:, :half], conv_taps[:, half:]
    taps = jnp.where(first, taps_low, taps_high)

    def mixed(gate, value, prev, mask):
        extended = jnp.concatenate([prev, gate], axis=0).astype(jnp.float32)
        near = mask[0][:, None] > 0.5
        far = mask[1][:, None] > 0.5
        conv = (
            taps[2] * extended[2:]
            + taps[1] * jnp.where(near, extended[1:-1], 0.0)
            + taps[0] * jnp.where(far, extended[:-2], 0.0)
        )
        return (jax.nn.silu(conv) * value.astype(jnp.float32)).astype(jnp.bfloat16)

    def lowered(gate, value, prev, mask):
        terms = down_product(mixed(gate, value, prev, mask), down_blocks)
        share = lax.psum_scatter(terms, "tp", scatter_dimension=0, tiled=True)
        return share.transpose(1, 0, 2).reshape(tokens, local_cols)

    down_theirs = flip(lowered(gate_theirs, value_both[tokens:], prev_theirs, masks_theirs), across)
    down_mine = lowered(gate_mine, value_both[:tokens], prev_mine, masks)
    down = down_mine.astype(jnp.float32) + down_theirs.astype(jnp.float32)
    return (residual_own + down).astype(jnp.bfloat16)


def next_pairs(count, across):
    pairs = []
    for s in range(count):
        column, top = s % across, s // (2 * across)
        if column < across - 1:
            pairs.append((s, s + 1))
        elif (top + 1) * 2 * across < count:
            pairs.append((s, s - column + 2 * across))
    return pairs


def solution(mesh):
    placed = (
        P("sp", "tp"),
        P("sp", "tp"),
        P("sp", "tp"),
        P("sp", "tp"),
        P("sp", "tp"),
        P("tp", "sp"),
        P("tp", "sp"),
        P("sp"),
        P("tp"),
        P("tp", None),
        P(),
        P("sp", "tp"),
        P("sp", "tp"),
        P(None, "tp"),
        P("tp", "sp"),
    )
    return jax.shard_map(layer, mesh=mesh, in_specs=placed, out_specs=P("sp", "tp"), check_vma=False)
```
